32 devices in a mesh: grp: 2 (over x), ep: 4 (over y, core), tp: 4 (over z).
Axes of the slice: x: 2, y: 2, z: 4, core: 2. Of those that a mesh axis runs over, the one named last changes fastest.
Arguments:
- tokens: bfloat16 [3072, 4096], P(('grp', 'ep'), 'tp'), parts along dimension 0
- pre_gain: float32 [4096], replicated, may hold values from 0.1 to 1.9
- out_gain: float32 [4096], P('tp'), may hold values from 0.1 to 1.9
- chosen: int32 [8, 4, 48], P(('grp', 'ep')), parts along dimension 0, may hold values from 0 to 383, as said below
- route_weight: float32 [8, 4, 48], P(('grp', 'ep')), parts along dimension 0, may hold values from 0.3 to 3
- expert_gate: bfloat16 [4, 4096, 3072], P('ep', None, 'tp'), may hold values from -0.09375 to 0.09375
- expert_up: bfloat16 [4, 4096, 3072], P('ep', None, 'tp'), may hold values from -0.09375 to 0.09375
- expert_down: bfloat16 [4, 3072, 4096], P('ep', 'tp'), may hold values from -0.109375 to 0.109375
Outputs:
- output: bfloat16 [3072, 4096], P(('grp', 'ep'), 'tp'), parts along dimension 0
The draws below stay inside these ranges and needn't reach their ends.
There are 2 independent parts, one for each index of `grp`. The reference program is written for one: setup_inputs(seed, part) draws one part's arguments, and reference() takes and returns one part's arrays. A program takes and returns all parts, laid end to end along the dimension named above; an argument that names none is the same for every part. Nothing has to cross between parts.
Inputs may be any that keep to these rules, and one draw needn't show every extreme that they name: chosen[b, e, k] is the position, within block b of 384 tokens, of the k-th token that expert e takes from that block; the 48 positions of one block and one expert are all different.
All inputs are finite; a program needn't handle non-finite values.
Results may differ from the reference program's by a relative error of at most 0.0075.
Values may be sent and summed in bfloat16 or wider, within the bound.
A program may use at most 64 MiB of HBM per device.

```python
import math
import jax
import jax.numpy as jnp
from jax import lax

D = 4096
FF = 3072
TOK_DEV = 384
SLOT = 48
BLOCKS = 4
EXPERTS = 4
CAP = 192
TOKENS = 1536
N_TP = 4


def draw_tokens(key, part):
    key_base, key_rough, key_rows = jax.random.split(jax.random.fold_in(key, 11), 3)
    rough = jnp.exp(jax.random.uniform(key_rough, (D,), jnp.float32, -0.4, 0.4))
    row_scale = 0.5 * jnp.exp(jax.random.uniform(key_rows, (TOKENS, 1), jnp.float32, 0.0, math.log(10.0)))
    column_scale = jnp.exp(jnp.linspace(0.0, math.log(4.0), D, dtype=jnp.float32))
    base = jax.random.normal(key_base, (TOKENS, D), jnp.float32)
    return (base * column_scale * rough * row_scale).astype(jnp.bfloat16)


def draw_chosen(key, part):
    shape_all = (BLOCKS, EXPERTS, TOK_DEV)
    scores = jax.random.randint(jax.random.fold_in(key, 7), shape_all, 0, 1 << 20)
    scores = scores * TOK_DEV + lax.broadcasted_iota(jnp.int32, shape_all, 2)
    ranking = jnp.argsort(scores, axis=-1)
    return ranking[..., :SLOT].astype(jnp.int32)


def level_of(stream_key, dims, cuts, least, high):
    def one(axis_at, blocks):
        steps = jax.random.uniform(jax.random.fold_in(jax.random.fold_in(stream_key, 6), axis_at), (blocks,), jnp.float32, least / len(cuts), high / len(cuts))
        return jnp.repeat(jnp.exp(steps), dims[axis_at] // blocks).reshape((-1,) + (1,) * (len(dims) - axis_at - 1))

    level = one(*cuts[0])
    for cut in cuts[1:]:
        level = level * one(*cut)
    return level


def noise(key, extent, spread, limit, pieces=(), held_as=jnp.bfloat16):
    entries = jax.random.normal(key, extent, jnp.float32) * spread
    if len(pieces) > 0:
        entries = level_of(key, extent, pieces, -0.22, 0.18) * entries
    return jnp.clip(entries, min=-limit, max=limit).astype(held_as)


def setup_inputs(seed: int = 0, part: int = 0) -> dict:
    key_of = jax.random.split(jax.random.key(seed), 9)
    part_keys = jax.random.split(jax.random.fold_in(key_of[8], part), 9)
    tokens = draw_tokens(jax.random.fold_in(jax.random.fold_in(key_of[8], part), 71), part)
    pre_gain = jnp.clip(1.0 + 0.18 * jax.random.normal(key_of[1], (D,), jnp.float32), 0.1, 1.9)
    out_gain = jnp.clip(1.0 + 0.18 * jax.random.normal(key_of[2], (D,), jnp.float32), 0.1, 1.9)
    chosen = draw_chosen(jax.random.fold_in(jax.random.fold_in(key_of[8], part), 71), part)
    route_weight = jnp.clip(jnp.exp(math.log(3.0) - 2.3025851 * jax.random.uniform(part_keys[4], (BLOCKS, EXPERTS, SLOT), jnp.float32) ** level_of(part_keys[4], (BLOCKS, EXPERTS, SLOT), ((0, 4),), -0.2, 0.2)), 0.3, 3.0)
    expert_gate = noise(key_of[5], (EXPERTS, D, FF), D ** -0.5, 0.09375, ((0, 4), (2, 4)))
    expert_up = noise(key_of[6], (EXPERTS, D, FF), D ** -0.5, 0.09375, ((0, 4), (2, 4)))
    expert_down = noise(key_of[7], (EXPERTS, FF, D), FF ** -0.5, 0.109375, ((0, 4), (1, 4)))
    return dict(tokens=tokens, pre_gain=pre_gain, out_gain=out_gain, chosen=chosen, route_weight=route_weight, expert_gate=expert_gate, expert_up=expert_up, expert_down=expert_down)


NORM_EPS = 1e-06

def reference(tokens, pre_gain, out_gain, chosen, route_weight, expert_gate, expert_up, expert_down):
    resident = tokens.astype(jnp.float32)
    row_scale = lax.rsqrt(lax.optimization_barrier(jnp.mean(resident * resident, axis=1, keepdims=True)) + NORM_EPS)
    normed = (resident * row_scale * pre_gain).astype(jnp.bfloat16)
    offsets = (jnp.arange(BLOCKS, dtype=jnp.int32) * TOK_DEV)[:, None, None]
    global_index = jnp.transpose(chosen + offsets, (1, 0, 2)).reshape(EXPERTS, CAP).astype(jnp.int32)
    weights_flat = jnp.transpose(route_weight, (1, 0, 2)).reshape(EXPERTS, CAP)
    group_width = FF // N_TP

    def one_expert(operands):
        index_row, gate_matrix, up_matrix, down_matrix = operands
        picked_rows = jnp.take(normed, index_row, axis=0)
        gate_act = jnp.dot(picked_rows, gate_matrix, preferred_element_type=jnp.float32)
        up_act = jnp.dot(picked_rows, up_matrix, preferred_element_type=jnp.float32)
        hidden = (jax.nn.silu(gate_act) * up_act).astype(jnp.bfloat16)
        grouped = hidden.astype(jnp.float32).reshape(CAP, N_TP, group_width)
        down_groups = down_matrix.astype(jnp.float32).reshape(N_TP, group_width, D)
        partial_terms = jnp.einsum('cng,ngd->ncd', grouped, down_groups, precision=lax.Precision.HIGHEST).astype(jnp.bfloat16)
        partial_terms = lax.optimization_barrier(partial_terms)
        return lax.optimization_barrier(jnp.sum(partial_terms.astype(jnp.float32), axis=0)).astype(jnp.bfloat16)
    expert_out = lax.map(one_expert, (global_index, expert_gate, expert_up, expert_down))
    contributions = expert_out.astype(jnp.float32) * weights_flat[:, :, None]
    update = jnp.zeros((TOKENS, D), jnp.float32).at[global_index.reshape(-1)].add(contributions.reshape(-1, D))
    mixed_rows = resident + update
    out_scale = lax.rsqrt(lax.optimization_barrier(jnp.mean(mixed_rows * mixed_rows, axis=1, keepdims=True)) + NORM_EPS)
    return (mixed_rows * out_scale * out_gain).astype(jnp.bfloat16)
```

```python
import functools

import jax
import jax.numpy as jnp
from jax import lax
from jax.experimental import pallas as pl
from jax.experimental.pallas import tpu as pltpu
from jax.sharding import PartitionSpec as P

NORM_EPS = 1e-06
MESH = pl.DeviceIdType.MESH
LANES = 128


def both(*conditions):
    held = conditions[0]
    for condition in conditions[1:]:
        held = jnp.logical_and(held, condition)
    return held


def line_order(place, count, step):
    near = jnp.minimum(place, count - 1 - place)
    reach = (step + 1) // 2
    inner = jnp.where(step % 2 == 1, place - reach, place + reach)
    outer = jnp.where(place < count - 1 - place, step, count - 1 - step)
    return jnp.where(step <= 2 * near, inner, outer)


def pair_of(here, count, chunk, sign):
    chips = count // 2
    chip, core = here // 2, here % 2
    far_chip = (chip + sign * ((chunk - 1) // 2 + 1) + 2 * chips) % chips
    far_core = jnp.where((chunk - 1) % 2 == 0, core, 1 - core)
    far = far_chip * 2 + far_core
    far = jnp.where(chunk == count - 1, chip * 2 + 1 - core, far)
    return jnp.where(chunk == 0, here, far)


def layer_kernel(
    n_ep, n_tp, model_width,
    tokens_ref, pre_gain_ref, out_gain_ref, chosen_ref, weight_ref, gate_hbm, up_hbm, down_hbm,
    out_ref,
    gate_w, up_w, down_w, rows, picked, part, carried, landed, gate_acc, up_acc, square_acc, hidden_ref,
    leaving, returned, mixed, sums_out, sums_in,
    gate_sem, up_sem, down_sem, pick_send, pick_recv, row_send, row_recv, part_send, part_recv,
    back_send, back_recv, sum_send, sum_recv,
):
    grp, me, at = lax.axis_index("grp"), lax.axis_index("ep"), lax.axis_index("tp")
    tok_count, width = tokens_ref.shape
    slots = chosen_ref.shape[2]
    last = n_tp - 1

    barrier = pltpu.get_barrier_semaphore()
    for step in range(1, n_tp):
        pl.semaphore_signal(barrier, inc=1, device_id=(grp, me, (at + step) % n_tp), device_id_type=MESH)
    for step in range(1, n_ep):
        pl.semaphore_signal(barrier, inc=1, device_id=(grp, (me + step) % n_ep, at), device_id_type=MESH)

    def load_gate(s):
        return pltpu.make_async_copy(gate_hbm.at[0, pl.ds(pl.multiple_of(s * width, width), width)], gate_w.at[s], gate_sem.at[s])

    def load_up(s):
        return pltpu.make_async_copy(up_hbm.at[0, pl.ds(pl.multiple_of(s * width, width), width)], up_w.at[s], up_sem.at[s])

    def load_down(s):
        return pltpu.make_async_copy(down_hbm.at[0, :, pl.ds(pl.multiple_of(s * width, width), width)], down_w.at[s], down_sem.at[s])

    @pl.loop(0, n_tp)
    def _(step):
        s = line_order(at, n_tp, step)
        load_gate(s).start()
        load_up(s).start()

    @pl.loop(0, n_tp)
    def _(step):
        load_down(line_order(at, n_tp, last - step)).start()

    def remote(src, dst, send, recv, ep_index, tp_index):
        return pltpu.make_async_remote_copy(
            src_ref=src, dst_ref=dst, send_sem=send, recv_sem=recv,
            device_id=(grp, ep_index, tp_index), device_id_type=MESH,
        )

    def pick_copy(c):
        return remote(picked.at[c], rows.at[c, at], pick_send.at[c], pick_recv.at[c], pair_of(me, n_ep, c, -1), at)

    def row_copy(c, s, right):
        return remote(
            rows.at[c, s], rows.at[c, s], row_send.at[right, c, s], row_recv.at[c, s],
            me, jnp.clip(at + (2 * right - 1), 0, last),
        )

    def part_copy(c, d, right):
        return remote(
            carried.at[c, d], landed.at[1 - right, c, d], part_send.at[c, d], part_recv.at[1 - right, c, d],
            me, jnp.clip(at + (2 * right - 1), 0, last),
        )

    def part_wait(c, d, side):
        remote(carried.at[c, d], landed.at[side, c, d], part_send.at[c, d], part_recv.at[side, c, d],
               me, jnp.clip(at + (2 * side - 1), 0, last)).wait_recv()

    def back_copy(c):
        return remote(leaving.at[c], returned.at[c], back_send.at[c], back_recv.at[c], pair_of(me, n_ep, c, 1), at)

    def sum_copy(step):
        return remote(sums_out, sums_in.at[at], sum_send.at[step], sum_recv.at[at], me, (at + step) % n_tp)

    place_of = lax.broadcasted_iota(jnp.int32, (tok_count, slots), 0)

    def pick(c):
        expert = pair_of(me, n_ep, c, -1)
        one_hot = jnp.where(place_of == chosen_ref[0, pl.ds(expert, 1), :], 1.0, 0.0).astype(jnp.bfloat16)
        return lax.dot_general(
            one_hot, tokens_ref[...], (((0,), (0,)), ((), ())), preferred_element_type=jnp.float32
        ).astype(jnp.bfloat16)

    def send_row(c, s):
        @pl.when(both(s <= at, at < last))
        def _():
            row_copy(c, s, 1).start()

        @pl.when(both(s >= at, at > 0))
        def _():
            row_copy(c, s, 0).start()

    rows[0, at] = pick(0)
    pl.semaphore_wait(barrier, n_tp - 1 + n_ep - 1)
    send_row(0, at)

    @pl.loop(1, n_ep)
    def _(c):
        picked[c] = pick(c)
        pick_copy(c).start()

    mixed[...] = tokens_ref[...].astype(jnp.float32)

    def multiply(c, step):
        s = line_order(at, n_tp, step)

        @pl.when(step > 0)
        def _():
            row_copy(c, s, 1).wait_recv()
            send_row(c, s)

        @pl.when(c == 0)
        def _():
            load_gate(s).wait()
            load_up(s).wait()

        raw = rows[c, s].astype(jnp.float32)
        scaled = (raw * pre_gain_ref[:, pl.ds(pl.multiple_of(s * width, width), width)]).astype(jnp.bfloat16)
        gate_acc[...] += jnp.dot(scaled, gate_w[s], preferred_element_type=jnp.float32)
        up_acc[...] += jnp.dot(scaled, up_w[s], preferred_element_type=jnp.float32)
        square_acc[...] += jnp.sum(raw * raw, axis=1, keepdims=True)

    def first_hop(d):
        return jnp.logical_or(both(at == 0, d > at), both(at == last, d < at))

    def start_part(c, d):
        @pl.when(d > at)
        def _():
            part_copy(c, d, 1).start()

        @pl.when(d < at)
        def _():
            part_copy(c, d, 0).start()

    def project(c, step):
        d = line_order(at, n_tp, last - step)

        @pl.when(c == 0)
        def _():
            load_down(d).wait()

        term = jnp.dot(hidden_ref[...], down_w[d], preferred_element_type=jnp.float32)
        part[c, d] = term

        @pl.when(first_hop(d))
        def _():
            carried[c, d] = part[c, d].astype(jnp.bfloat16)
            start_part(c, d)

    def relay(c):
        @pl.loop(0, last)
        def _(step):
            d = line_order(at, n_tp, last - step)

            @pl.when(jnp.logical_not(first_hop(d)))
            def _():
                side = jnp.where(d > at, 0, 1)
                part_wait(c, d, side)
                carried[c, d] = (part[c, d] + landed[side, c, d].astype(jnp.float32)).astype(jnp.bfloat16)
                start_part(c, d)

    def finish(c):
        @pl.when(at > 0)
        def _():
            part_wait(c, at, 0)
            part[c, at] += landed[0, c, at].astype(jnp.float32)

        @pl.when(at < last)
        def _():
            part_wait(c, at, 1)
            part[c, at] += landed[1, c, at].astype(jnp.float32)

        @pl.when(c == 0)
        def _():
            returned[0] = part[0, at].astype(jnp.bfloat16)

        @pl.when(c > 0)
        def _():
            leaving[c] = part[c, at].astype(jnp.bfloat16)
            back_copy(c).start()

    def scatter(c):
        @pl.when(c > 0)
        def _():
            back_copy(c).wait_recv()

        expert = pair_of(me, n_ep, c, -1)
        weight = weight_ref[0, pl.ds(expert, 1), :]
        coarse = weight.astype(jnp.bfloat16).astype(jnp.float32)
        here = place_of == chosen_ref[0, pl.ds(expert, 1), :]
        spread = jnp.where(here, coarse, 0.0).astype(jnp.bfloat16)
        fine = jnp.where(here, weight - coarse, 0.0).astype(jnp.bfloat16)
        block = returned[c]
        mixed[...] += jnp.dot(spread, block, preferred_element_type=jnp.float32) + jnp.dot(
            fine, block, preferred_element_type=jnp.float32
        )

    @pl.loop(0, n_ep)
    def _(c):
        gate_acc[...] = jnp.zeros_like(gate_acc)
        up_acc[...] = jnp.zeros_like(up_acc)
        square_acc[...] = jnp.zeros_like(square_acc)

        @pl.loop(0, n_tp)
        def _(step):
            multiply(c, step)

            @pl.when(both(step == 0, c + 1 < n_ep))
            def _():
                pick_copy(c + 1).wait_recv()
                send_row(c + 1, at)

        scale = lax.rsqrt(square_acc[...] / model_width + NORM_EPS)
        gate = gate_acc[...] * scale
        hidden_ref[...] = (gate / (1.0 + jnp.exp(-gate)) * (up_acc[...] * scale)).astype(jnp.bfloat16)

        @pl.loop(0, n_tp)
        def _(step):
            project(c, step)

        @pl.when(c >= 1)
        def _():
            relay(c - 1)

        @pl.when(c >= 2)
        def _():
            finish(c - 2)

    if n_ep >= 2:
        finish(n_ep - 2)

    @pl.loop(0, n_ep - 2)
    def _(c):
        scatter(c)

    relay(n_ep - 1)
    if n_ep >= 2:
        scatter(n_ep - 2)
    finish(n_ep - 1)
    scatter(n_ep - 1)

    square = mixed[...] * mixed[...]
    lanes = square[:, :LANES]
    for k in range(1, width // LANES):
        lanes = lanes + square[:, k * LANES:(k + 1) * LANES]
    mine = jnp.sum(lanes.T, axis=0, keepdims=True)
    sums_out[...] = jnp.broadcast_to(mine, sums_out.shape)
    for step in range(1, n_tp):
        sum_copy(step).start()
    total = sums_out[...]
    for step in range(1, n_tp):
        source = (at + step) % n_tp
        remote(sums_out, sums_in.at[source], sum_send.at[step], sum_recv.at[source], me, source).wait_recv()
        total = total + sums_in[source]
    scale = lax.rsqrt(total / model_width + NORM_EPS)
    column = jnp.concatenate([scale] * (LANES // scale.shape[0]), axis=0).T
    for k in range(width // LANES):
        span = slice(k * LANES, (k + 1) * LANES)
        out_ref[:, span] = (mixed[:, span] * column * out_gain_ref[:, span]).astype(out_ref.dtype)

    for step in range(1, n_tp):
        sum_copy(step).wait_send()

    @pl.loop(0, n_ep)
    def _(c):
        @pl.when(c > 0)
        def _():
            pick_copy(c).wait_send()
            back_copy(c).wait_send()

        @pl.loop(0, n_tp)
        def _(s):
            @pl.when(both(s <= at, at < last))
            def _():
                row_copy(c, s, 1).wait_send()

            @pl.when(both(s >= at, at > 0))
            def _():
                row_copy(c, s, 0).wait_send()

            @pl.when(s > at)
            def _():
                part_copy(c, s, 1).wait_send()

            @pl.when(s < at)
            def _():
                part_copy(c, s, 0).wait_send()


def solution(mesh):
    n_ep, n_tp = mesh.shape["ep"], mesh.shape["tp"]

    def shards(tokens, pre_gain, out_gain, chosen, route_weight, expert_gate, expert_up, expert_down):
        tok_count, width = tokens.shape
        model_width = pre_gain.shape[0]
        slots, units = chosen.shape[2], expert_gate.shape[2]
        bf16, f32 = jnp.bfloat16, jnp.float32
        dma = pltpu.SemaphoreType.DMA
        vmem = pl.BlockSpec(memory_space=pltpu.VMEM)
        hbm = pl.BlockSpec(memory_space=pl.ANY)
        return pl.pallas_call(
            functools.partial(layer_kernel, n_ep, n_tp, model_width),
            out_shape=jax.ShapeDtypeStruct((tok_count, width), bf16),
            in_specs=[vmem] * 5 + [hbm] * 3,
            out_specs=vmem,
            scratch_shapes=[
                pltpu.VMEM((n_tp, width, units), bf16),
                pltpu.VMEM((n_tp, width, units), bf16),
                pltpu.VMEM((n_tp, units, width), bf16),
                pltpu.VMEM((n_ep, n_tp, slots, width), bf16),
                pltpu.VMEM((n_ep, slots, width), bf16),
                pltpu.VMEM((n_ep, n_tp, slots, width), f32),
                pltpu.VMEM((n_ep, n_tp, slots, width), bf16),
                pltpu.VMEM((2, n_ep, n_tp, slots, width), bf16),
                pltpu.VMEM((slots, units), f32),
                pltpu.VMEM((slots, units), f32),
                pltpu.VMEM((slots, 1), f32),
                pltpu.VMEM((slots, units), bf16),
                pltpu.VMEM((n_ep, slots, width), bf16),
                pltpu.VMEM((n_ep, slots, width), bf16),
                pltpu.VMEM((tok_count, width), f32),
                pltpu.VMEM((8, tok_count), f32),
                pltpu.VMEM((n_tp, 8, tok_count), f32),
                dma((n_tp,)), dma((n_tp,)), dma((n_tp,)),
                dma((n_ep,)), dma((n_ep,)),
                dma((2, n_ep, n_tp)), dma((n_ep, n_tp)),
                dma((n_ep, n_tp)), dma((2, n_ep, n_tp)),
                dma((n_ep,)), dma((n_ep,)),
                dma((n_tp,)), dma((n_tp,)),
            ],
            compiler_params=pltpu.CompilerParams(
                collective_id=0, has_side_effects=True, vmem_limit_bytes=67043328
            ),
        )(
            tokens, pre_gain.reshape(1, -1), out_gain.reshape(1, -1), chosen, route_weight,
            expert_gate, expert_up, expert_down,
        )

    return jax.shard_map(
        shards,
        mesh=mesh,
        in_specs=(
            P(("grp", "ep"), "tp"),
            P(),
            P("tp"),
            P(("grp", "ep"), None, None),
            P(("grp", "ep"), None, None),
            P("ep", None, "tp"),
            P("ep", None, "tp"),
            P("ep", "tp", None),
        ),
        out_specs=P(("grp", "ep"), "tp"),
        check_vma=False,
    )
```

```python
import functools

import jax
import jax.numpy as jnp
from jax import lax
from jax.experimental import pallas as pl
from jax.experimental.pallas import tpu as pltpu
from jax.sharding import PartitionSpec as P

NORM_EPS = 1e-06
MESH = pl.DeviceIdType.MESH
LANES = 128
PIECES = 2


def both(*conditions):
    held = conditions[0]
    for condition in conditions[1:]:
        held = jnp.logical_and(held, condition)
    return held


def line_order(place, count, step):
    near = jnp.minimum(place, count - 1 - place)
    reach = (step + 1) // 2
    inner = jnp.where(step % 2 == 1, place - reach, place + reach)
    outer = jnp.where(place < count - 1 - place, step, count - 1 - step)
    return jnp.where(step <= 2 * near, inner, outer)


def pair_of(here, count, chunk, sign):
    chips = count // 2
    chip, core = here // 2, here % 2
    far_chip = (chip + sign * ((chunk - 1) // 2 + 1) + 2 * chips) % chips
    far_core = jnp.where((chunk - 1) % 2 == 0, core, 1 - core)
    far = far_chip * 2 + far_core
    far = jnp.where(chunk == count - 1, chip * 2 + 1 - core, far)
    return jnp.where(chunk == 0, here, far)


def layer_kernel(
    n_ep, n_tp, model_width,
    tokens_ref, pre_gain_ref, out_gain_ref, chosen_ref, weight_ref, gate_hbm, up_hbm, down_hbm,
    out_ref,
    gate_w, up_w, down_w, rows, picked, part, carried, landed, gate_acc, up_acc, square_acc, hidden_ref,
    leaving, returned, mixed, sums_out, sums_in,
    gate_sem, up_sem, down_sem, pick_send, pick_recv, row_send, row_recv, part_send, part_recv,
    back_send, back_recv, sum_send, sum_recv,
):
    grp, me, at = lax.axis_index("grp"), lax.axis_index("ep"), lax.axis_index("tp")
    tok_count, width = tokens_ref.shape
    slots = chosen_ref.shape[2]
    last = n_tp - 1
    pieces, narrow = down_w.shape[1], down_w.shape[3]

    barrier = pltpu.get_barrier_semaphore()
    for step in range(1, n_tp):
        pl.semaphore_signal(barrier, inc=1, device_id=(grp, me, (at + step) % n_tp), device_id_type=MESH)
    for step in range(1, n_ep):
        pl.semaphore_signal(barrier, inc=1, device_id=(grp, (me + step) % n_ep, at), device_id_type=MESH)

    def load_gate(s):
        return pltpu.make_async_copy(gate_hbm.at[0, pl.ds(pl.multiple_of(s * width, width), width)], gate_w.at[s], gate_sem.at[s])

    def load_up(s):
        return pltpu.make_async_copy(up_hbm.at[0, pl.ds(pl.multiple_of(s * width, width), width)], up_w.at[s], up_sem.at[s])

    def load_down(s, h):
        span = pl.ds(pl.multiple_of((s * pieces + h) * narrow, narrow), narrow)
        return pltpu.make_async_copy(down_hbm.at[0, :, span], down_w.at[s, h], down_sem.at[s, h])

    @pl.loop(0, n_tp)
    def _(step):
        s = line_order(at, n_tp, step)
        load_gate(s).start()
        load_up(s).start()

    @pl.loop(0, n_tp)
    def _(step):
        for h in range(pieces):
            load_down(line_order(at, n_tp, last - step), h).start()

    def remote(src, dst, send, recv, ep_index, tp_index):
        return pltpu.make_async_remote_copy(
            src_ref=src, dst_ref=dst, send_sem=send, recv_sem=recv,
            device_id=(grp, ep_index, tp_index), device_id_type=MESH,
        )

    def pick_copy(c):
        return remote(picked.at[c], rows.at[c, at], pick_send.at[c], pick_recv.at[c], pair_of(me, n_ep, c, -1), at)

    def row_copy(c, s, right):
        return remote(
            rows.at[c, s], rows.at[c, s], row_send.at[right, c, s], row_recv.at[c, s],
            me, jnp.clip(at + (2 * right - 1), 0, last),
        )

    def part_copy(c, d, h, right):
        return remote(
            carried.at[c, d, h], landed.at[1 - right, c, d, h],
            part_send.at[c, d, h], part_recv.at[1 - right, c, d, h],
            me, jnp.clip(at + (2 * right - 1), 0, last),
        )

    def part_wait(c, d, h, side):
        remote(carried.at[c, d, h], landed.at[side, c, d, h], part_send.at[c, d, h], part_recv.at[side, c, d, h],
               me, jnp.clip(at + (2 * side - 1), 0, last)).wait_recv()

    def back_copy(c, h):
        return remote(
            leaving.at[c, h], returned.at[c, h], back_send.at[c, h], back_recv.at[c, h], pair_of(me, n_ep, c, 1), at
        )

    def sum_copy(step):
        return remote(sums_out, sums_in.at[at], sum_send.at[step], sum_recv.at[at], me, (at + step) % n_tp)

    place_of = lax.broadcasted_iota(jnp.int32, (tok_count, slots), 0)

    def pick(c):
        expert = pair_of(me, n_ep, c, -1)
        one_hot = jnp.where(place_of == chosen_ref[0, pl.ds(expert, 1), :], 1.0, 0.0).astype(jnp.bfloat16)
        return lax.dot_general(
            one_hot, tokens_ref[...], (((0,), (0,)), ((), ())), preferred_element_type=jnp.float32
        ).astype(jnp.bfloat16)

    def send_row(c, s):
        @pl.when(both(s <= at, at < last))
        def _():
            row_copy(c, s, 1).start()

        @pl.when(both(s >= at, at > 0))
        def _():
            row_copy(c, s, 0).start()

    rows[0, at] = pick(0)
    pl.semaphore_wait(barrier, n_tp - 1 + n_ep - 1)
    send_row(0, at)

    @pl.loop(1, n_ep)
    def _(c):
        picked[c] = pick(c)
        pick_copy(c).start()

    mixed[...] = tokens_ref[...].astype(jnp.float32)

    def pass_on(slot):
        @pl.when(both(slot % n_tp > 0, slot < n_ep * n_tp))
        def _():
            c = slot // n_tp
            s = line_order(at, n_tp, slot % n_tp)
            row_copy(c, s, 1).wait_recv()
            send_row(c, s)

    def start_own(slot):
        @pl.when(both(slot % n_tp == 0, slot < n_ep * n_tp))
        def _():
            c = slot // n_tp
            pick_copy(c).wait_recv()
            send_row(c, at)

    def multiply(c, step):
        s = line_order(at, n_tp, step)

        @pl.when(c == 0)
        def _():
            load_gate(s).wait()
            load_up(s).wait()

        raw = rows[c, s].astype(jnp.float32)
        scaled = (raw * pre_gain_ref[:, pl.ds(pl.multiple_of(s * width, width), width)]).astype(jnp.bfloat16)
        gate_acc[...] += jnp.dot(scaled, gate_w[s], preferred_element_type=jnp.float32)
        up_acc[...] += jnp.dot(scaled, up_w[s], preferred_element_type=jnp.float32)
        square_acc[...] += jnp.sum(raw * raw, axis=1, keepdims=True)

    def first_hop(d):
        return jnp.logical_or(both(at == 0, d > at), both(at == last, d < at))

    def start_part(c, d, h):
        @pl.when(d > at)
        def _():
            part_copy(c, d, h, 1).start()

        @pl.when(d < at)
        def _():
            part_copy(c, d, h, 0).start()

    def project(c, step):
        d = line_order(at, n_tp, last - step)

        for h in range(pieces):
            @pl.when(c == 0)
            def _():
                load_down(d, h).wait()

            part[c, d, h] = jnp.dot(hidden_ref[...], down_w[d, h], preferred_element_type=jnp.float32)

            @pl.when(first_hop(d))
            def _():
                carried[c, d, h] = part[c, d, h].astype(jnp.bfloat16)
                start_part(c, d, h)

    def second_hop(d):
        return jnp.logical_or(both(at == 1, d > at), both(at == last - 1, d < at))

    def relay(c, early):
        @pl.loop(0, last)
        def _(step):
            d = line_order(at, n_tp, last - step)
            wanted = second_hop(d) if early else jnp.logical_not(second_hop(d))

            @pl.when(both(wanted, jnp.logical_not(first_hop(d))))
            def _():
                side = jnp.where(d > at, 0, 1)
                for h in range(pieces):
                    part_wait(c, d, h, side)
                    carried[c, d, h] = (part[c, d, h] + landed[side, c, d, h].astype(jnp.float32)).astype(jnp.bfloat16)
                    start_part(c, d, h)

    def finish(c):
        for h in range(pieces):
            @pl.when(at > 0)
            def _():
                part_wait(c, at, h, 0)
                part[c, at, h] += landed[0, c, at, h].astype(jnp.float32)

            @pl.when(at < last)
            def _():
                part_wait(c, at, h, 1)
                part[c, at, h] += landed[1, c, at, h].astype(jnp.float32)

            @pl.when(c == 0)
            def _():
                returned[0, h] = part[0, at, h].astype(jnp.bfloat16)

            @pl.when(c > 0)
            def _():
                leaving[c, h] = part[c, at, h].astype(jnp.bfloat16)
                back_copy(c, h).start()

    def scatter(c):
        expert = pair_of(me, n_ep, c, -1)
        weight = weight_ref[0, pl.ds(expert, 1), :]
        coarse = weight.astype(jnp.bfloat16).astype(jnp.float32)
        here = place_of == chosen_ref[0, pl.ds(expert, 1), :]
        spread = jnp.where(here, coarse, 0.0).astype(jnp.bfloat16)
        fine = jnp.where(here, weight - coarse, 0.0).astype(jnp.bfloat16)
        for h in range(pieces):
            @pl.when(c > 0)
            def _():
                back_copy(c, h).wait_recv()

            block = returned[c, h]
            mixed[:, h * narrow:(h + 1) * narrow] += jnp.dot(
                spread, block, preferred_element_type=jnp.float32
            ) + jnp.dot(fine, block, preferred_element_type=jnp.float32)

    @pl.loop(0, n_ep)
    def _(c):
        gate_acc[...] = jnp.zeros_like(gate_acc)
        up_acc[...] = jnp.zeros_like(up_acc)
        square_acc[...] = jnp.zeros_like(square_acc)

        @pl.loop(0, n_tp)
        def _(step):
            slot = c * n_tp + step
            pass_on(slot)
            multiply(c, step)
            start_own(slot + n_tp + 1)

            @pl.when(slot == 0)
            def _():
                start_own(n_tp)

        scale = lax.rsqrt(square_acc[...] / model_width + NORM_EPS)
        gate = gate_acc[...] * scale
        hidden_ref[...] = (gate / (1.0 + jnp.exp(-gate)) * (up_acc[...] * scale)).astype(jnp.bfloat16)

        @pl.loop(0, n_tp)
        def _(step):
            project(c, step)

        @pl.when(c >= 1)
        def _():
            relay(c - 1, True)

    @pl.loop(0, n_ep - 1)
    def _(c):
        relay(c, False)

    relay(n_ep - 1, True)

    @pl.loop(0, n_ep - 1)
    def _(c):
        finish(c)

    relay(n_ep - 1, False)

    @pl.loop(0, n_ep - 1)
    def _(c):
        scatter(c)

    finish(n_ep - 1)
    scatter(n_ep - 1)

    square = mixed[...] * mixed[...]
    lanes = square[:, :LANES]
    for k in range(1, width // LANES):
        lanes = lanes + square[:, k * LANES:(k + 1) * LANES]
    mine = jnp.sum(lanes.T, axis=0, keepdims=True)
    sums_out[...] = jnp.broadcast_to(mine, sums_out.shape)
    for step in range(1, n_tp):
        sum_copy(step).start()
    total = sums_out[...]
    for step in range(1, n_tp):
        source = (at + step) % n_tp
        remote(sums_out, sums_in.at[source], sum_send.at[step], sum_recv.at[source], me, source).wait_recv()
        total = total + sums_in[source]
    scale = lax.rsqrt(total / model_width + NORM_EPS)
    column = jnp.concatenate([scale] * (LANES // scale.shape[0]), axis=0).T
    for k in range(width // LANES):
        span = slice(k * LANES, (k + 1) * LANES)
        out_ref[:, span] = (mixed[:, span] * column * out_gain_ref[:, span]).astype(out_ref.dtype)

    for step in range(1, n_tp):
        sum_copy(step).wait_send()

    @pl.loop(0, n_ep)
    def _(c):
        @pl.when(c > 0)
        def _():
            pick_copy(c).wait_send()
            for h in range(pieces):
                back_copy(c, h).wait_send()

        @pl.loop(0, n_tp)
        def _(s):
            @pl.when(both(s <= at, at < last))
            def _():
                row_copy(c, s, 1).wait_send()

            @pl.when(both(s >= at, at > 0))
            def _():
                row_copy(c, s, 0).wait_send()

            for h in range(pieces):
                @pl.when(s > at)
                def _():
                    part_copy(c, s, h, 1).wait_send()

                @pl.when(s < at)
                def _():
                    part_copy(c, s, h, 0).wait_send()


def solution(mesh):
    n_ep, n_tp = mesh.shape["ep"], mesh.shape["tp"]

    def shards(tokens, pre_gain, out_gain, chosen, route_weight, expert_gate, expert_up, expert_down):
        tok_count, width = tokens.shape
        model_width = pre_gain.shape[0]
        slots, units = chosen.shape[2], expert_gate.shape[2]
        narrow = width // PIECES
        bf16, f32 = jnp.bfloat16, jnp.float32
        dma = pltpu.SemaphoreType.DMA
        vmem = pl.BlockSpec(memory_space=pltpu.VMEM)
        hbm = pl.BlockSpec(memory_space=pl.ANY)
        return pl.pallas_call(
            functools.partial(layer_kernel, n_ep, n_tp, model_width),
            out_shape=jax.ShapeDtypeStruct((tok_count, width), bf16),
            in_specs=[vmem] * 5 + [hbm] * 3,
            out_specs=vmem,
            scratch_shapes=[
                pltpu.VMEM((n_tp, width, units), bf16),
                pltpu.VMEM((n_tp, width, units), bf16),
                pltpu.VMEM((n_tp, PIECES, units, narrow), bf16),
                pltpu.VMEM((n_ep, n_tp, slots, width), bf16),
                pltpu.VMEM((n_ep, slots, width), bf16),
                pltpu.VMEM((n_ep, n_tp, PIECES, slots, narrow), f32),
                pltpu.VMEM((n_ep, n_tp, PIECES, slots, narrow), bf16),
                pltpu.VMEM((2, n_ep, n_tp, PIECES, slots, narrow), bf16),
                pltpu.VMEM((slots, units), f32),
                pltpu.VMEM((slots, units), f32),
                pltpu.VMEM((slots, 1), f32),
                pltpu.VMEM((slots, units), bf16),
                pltpu.VMEM((n_ep, PIECES, slots, narrow), bf16),
                pltpu.VMEM((n_ep, PIECES, slots, narrow), bf16),
                pltpu.VMEM((tok_count, width), f32),
                pltpu.VMEM((8, tok_count), f32),
                pltpu.VMEM((n_tp, 8, tok_count), f32),
                dma((n_tp,)), dma((n_tp,)), dma((n_tp, PIECES)),
                dma((n_ep,)), dma((n_ep,)),
                dma((2, n_ep, n_tp)), dma((n_ep, n_tp)),
                dma((n_ep, n_tp, PIECES)), dma((2, n_ep, n_tp, PIECES)),
                dma((n_ep, PIECES)), dma((n_ep, PIECES)),
                dma((n_tp,)), dma((n_tp,)),
            ],
            compiler_params=pltpu.CompilerParams(
                collective_id=0, has_side_effects=True, vmem_limit_bytes=67043328
            ),
        )(
            tokens, pre_gain.reshape(1, -1), out_gain.reshape(1, -1), chosen, route_weight,
            expert_gate, expert_up, expert_down,
        )

    return jax.shard_map(
        shards,
        mesh=mesh,
        in_specs=(
            P(("grp", "ep"), "tp"),
            P(),
            P("tp"),
            P(("grp", "ep"), None, None),
            P(("grp", "ep"), None, None),
            P("ep", None, "tp"),
            P("ep", None, "tp"),
            P("ep", "tp", None),
        ),
        out_specs=P(("grp", "ep"), "tp"),
        check_vma=False,
    )
```

```python
import functools

import jax
import jax.numpy as jnp
from jax import lax
from jax.experimental import pallas as pl
from jax.experimental.pallas import tpu as pltpu
from jax.sharding import PartitionSpec as P

NORM_EPS = 1e-06
MESH = pl.DeviceIdType.MESH
LANES = 128
PIECES = 1


def both(*conditions):
    held = conditions[0]
    for condition in conditions[1:]:
        held = jnp.logical_and(held, condition)
    return held


def line_order(place, count, step):
    near = jnp.minimum(place, count - 1 - place)
    reach = (step + 1) // 2
    inner = jnp.where(step % 2 == 1, place - reach, place + reach)
    outer = jnp.where(place < count - 1 - place, step, count - 1 - step)
    return jnp.where(step <= 2 * near, inner, outer)


def pair_of(here, count, chunk, sign):
    chips = count // 2
    chip, core = here // 2, here % 2
    far_chip = (chip + sign * ((chunk - 1) // 2 + 1) + 2 * chips) % chips
    far_core = jnp.where((chunk - 1) % 2 == 0, core, 1 - core)
    far = far_chip * 2 + far_core
    far = jnp.where(chunk == count - 1, chip * 2 + 1 - core, far)
    return jnp.where(chunk == 0, here, far)


def layer_kernel(
    n_ep, n_tp, model_width,
    tokens_ref, pre_gain_ref, out_gain_ref, chosen_ref, weight_ref, gate_hbm, up_hbm, down_hbm,
    out_ref,
    gate_w, up_w, down_w, rows, picked, part, carried, landed, gate_acc, up_acc, square_acc, hidden_ref,
    leaving, returned, mixed, sums_out, sums_in,
    gate_sem, up_sem, down_sem, pick_send, pick_recv, row_send, row_recv, part_send, part_recv,
    back_send, back_recv, sum_send, sum_recv,
):
    grp, me, at = lax.axis_index("grp"), lax.axis_index("ep"), lax.axis_index("tp")
    tok_count, width = tokens_ref.shape
    slots = chosen_ref.shape[2]
    last = n_tp - 1
    pieces, narrow = down_w.shape[1], down_w.shape[3]

    barrier = pltpu.get_barrier_semaphore()
    for step in range(1, n_tp):
        pl.semaphore_signal(barrier, inc=1, device_id=(grp, me, (at + step) % n_tp), device_id_type=MESH)
    for step in range(1, n_ep):
        pl.semaphore_signal(barrier, inc=1, device_id=(grp, (me + step) % n_ep, at), device_id_type=MESH)

    def load_gate(s):
        return pltpu.make_async_copy(gate_hbm.at[0, pl.ds(pl.multiple_of(s * width, width), width)], gate_w.at[s], gate_sem.at[s])

    def load_up(s):
        return pltpu.make_async_copy(up_hbm.at[0, pl.ds(pl.multiple_of(s * width, width), width)], up_w.at[s], up_sem.at[s])

    def load_down(s, h):
        span = pl.ds(pl.multiple_of((s * pieces + h) * narrow, narrow), narrow)
        return pltpu.make_async_copy(down_hbm.at[0, :, span], down_w.at[s, h], down_sem.at[s, h])

    @pl.loop(0, n_tp)
    def _(step):
        s = line_order(at, n_tp, step)
        load_gate(s).start()
        load_up(s).start()

    @pl.loop(0, n_tp)
    def _(step):
        for h in range(pieces):
            load_down(line_order(at, n_tp, last - step), h).start()

    def remote(src, dst, send, recv, ep_index, tp_index):
        return pltpu.make_async_remote_copy(
            src_ref=src, dst_ref=dst, send_sem=send, recv_sem=recv,
            device_id=(grp, ep_index, tp_index), device_id_type=MESH,
        )

    def pick_copy(c):
        return remote(picked.at[c], rows.at[c, at], pick_send.at[c], pick_recv.at[c], pair_of(me, n_ep, c, -1), at)

    def row_copy(c, s, right):
        return remote(
            rows.at[c, s], rows.at[c, s], row_send.at[right, c, s], row_recv.at[c, s],
            me, jnp.clip(at + (2 * right - 1), 0, last),
        )

    def part_copy(c, d, h, right):
        return remote(
            carried.at[c, d, h], landed.at[1 - right, c, d, h],
            part_send.at[c, d, h], part_recv.at[1 - right, c, d, h],
            me, jnp.clip(at + (2 * right - 1), 0, last),
        )

    def part_wait(c, d, h, side):
        remote(carried.at[c, d, h], landed.at[side, c, d, h], part_send.at[c, d, h], part_recv.at[side, c, d, h],
               me, jnp.clip(at + (2 * side - 1), 0, last)).wait_recv()

    def back_copy(c, h):
        return remote(
            leaving.at[c, h], returned.at[c, h], back_send.at[c, h], back_recv.at[c, h], pair_of(me, n_ep, c, 1), at
        )

    def sum_copy(step):
        return remote(sums_out, sums_in.at[at], sum_send.at[step], sum_recv.at[at], me, (at + step) % n_tp)

    place_of = lax.broadcasted_iota(jnp.int32, (tok_count, slots), 0)

    def pick(c):
        expert = pair_of(me, n_ep, c, -1)
        one_hot = jnp.where(place_of == chosen_ref[0, pl.ds(expert, 1), :], 1.0, 0.0).astype(jnp.bfloat16)
        return lax.dot_general(
            one_hot, tokens_ref[...], (((0,), (0,)), ((), ())), preferred_element_type=jnp.float32
        ).astype(jnp.bfloat16)

    def send_row(c, s):
        @pl.when(both(s <= at, at < last))
        def _():
            row_copy(c, s, 1).start()

        @pl.when(both(s >= at, at > 0))
        def _():
            row_copy(c, s, 0).start()

    rows[0, at] = pick(0)
    pl.semaphore_wait(barrier, n_tp - 1 + n_ep - 1)
    send_row(0, at)

    @pl.loop(1, n_ep)
    def _(c):
        picked[c] = pick(c)
        pick_copy(c).start()

    mixed[...] = tokens_ref[...].astype(jnp.float32)

    def pass_on(slot):
        @pl.when(both(slot % n_tp > 0, slot < n_ep * n_tp))
        def _():
            c = slot // n_tp
            s = line_order(at, n_tp, slot % n_tp)
            row_copy(c, s, 1).wait_recv()
            send_row(c, s)

    def start_own(slot):
        @pl.when(both(slot % n_tp == 0, slot < n_ep * n_tp))
        def _():
            c = slot // n_tp
            pick_copy(c).wait_recv()
            send_row(c, at)

    def multiply(c, step):
        s = line_order(at, n_tp, step)

        @pl.when(c == 0)
        def _():
            load_gate(s).wait()
            load_up(s).wait()

        raw = rows[c, s].astype(jnp.float32)
        scaled = (raw * pre_gain_ref[:, pl.ds(pl.multiple_of(s * width, width), width)]).astype(jnp.bfloat16)
        gate_acc[...] += jnp.dot(scaled, gate_w[s], preferred_element_type=jnp.float32)
        up_acc[...] += jnp.dot(scaled, up_w[s], preferred_element_type=jnp.float32)
        square_acc[...] += jnp.sum(raw * raw, axis=1, keepdims=True)

    def first_hop(d):
        return jnp.logical_or(both(at == 0, d > at), both(at == last, d < at))

    def start_part(c, d, h):
        @pl.when(d > at)
        def _():
            part_copy(c, d, h, 1).start()

        @pl.when(d < at)
        def _():
            part_copy(c, d, h, 0).start()

    def project(c, step):
        d = line_order(at, n_tp, last - step)

        for h in range(pieces):
            @pl.when(c == 0)
            def _():
                load_down(d, h).wait()

            part[c, d, h] = jnp.dot(hidden_ref[...], down_w[d, h], preferred_element_type=jnp.float32)

            @pl.when(first_hop(d))
            def _():
                carried[c, d, h] = part[c, d, h].astype(jnp.bfloat16)
                start_part(c, d, h)

    def second_hop(d):
        return jnp.logical_or(both(at == 1, d > at), both(at == last - 1, d < at))

    def relay(c, early):
        @pl.loop(0, last)
        def _(step):
            d = line_order(at, n_tp, last - step)
            wanted = second_hop(d) if early else jnp.logical_not(second_hop(d))

            @pl.when(both(wanted, jnp.logical_not(first_hop(d))))
            def _():
                side = jnp.where(d > at, 0, 1)
                for h in range(pieces):
                    part_wait(c, d, h, side)
                    carried[c, d, h] = (part[c, d, h] + landed[side, c, d, h].astype(jnp.float32)).astype(jnp.bfloat16)
                    start_part(c, d, h)

    def finish(c):
        for h in range(pieces):
            @pl.when(at > 0)
            def _():
                part_wait(c, at, h, 0)
                part[c, at, h] += landed[0, c, at, h].astype(jnp.float32)

            @pl.when(at < last)
            def _():
                part_wait(c, at, h, 1)
                part[c, at, h] += landed[1, c, at, h].astype(jnp.float32)

            @pl.when(c == 0)
            def _():
                returned[0, h] = part[0, at, h].astype(jnp.bfloat16)

            @pl.when(c > 0)
            def _():
                leaving[c, h] = part[c, at, h].astype(jnp.bfloat16)
                back_copy(c, h).start()

    def scatter(c):
        expert = pair_of(me, n_ep, c, -1)
        weight = weight_ref[0, pl.ds(expert, 1), :]
        coarse = weight.astype(jnp.bfloat16).astype(jnp.float32)
        here = place_of == chosen_ref[0, pl.ds(expert, 1), :]
        spread = jnp.where(here, coarse, 0.0).astype(jnp.bfloat16)
        fine = jnp.where(here, weight - coarse, 0.0).astype(jnp.bfloat16)
        for h in range(pieces):
            @pl.when(c > 0)
            def _():
                back_copy(c, h).wait_recv()

            block = returned[c, h]
            mixed[:, h * narrow:(h + 1) * narrow] += jnp.dot(
                spread, block, preferred_element_type=jnp.float32
            ) + jnp.dot(fine, block, preferred_element_type=jnp.float32)

    @pl.loop(0, n_ep)
    def _(c):
        gate_acc[...] = jnp.zeros_like(gate_acc)
        up_acc[...] = jnp.zeros_like(up_acc)
        square_acc[...] = jnp.zeros_like(square_acc)

        @pl.loop(0, n_tp)
        def _(step):
            slot = c * n_tp + step
            pass_on(slot)
            multiply(c, step)
            start_own(slot + n_tp + 1)

            @pl.when(slot == 0)
            def _():
                start_own(n_tp)

        scale = lax.rsqrt(square_acc[...] / model_width + NORM_EPS)
        gate = gate_acc[...] * scale
        hidden_ref[...] = (gate / (1.0 + jnp.exp(-gate)) * (up_acc[...] * scale)).astype(jnp.bfloat16)

        @pl.loop(0, n_tp)
        def _(step):
            project(c, step)

        @pl.when(c >= 2)
        def _():
            relay(c - 2, True)

    relay(n_ep - 2, True)

    @pl.loop(0, n_ep - 1)
    def _(c):
        relay(c, False)

    relay(n_ep - 1, True)

    @pl.loop(0, n_ep - 1)
    def _(c):
        finish(c)

    relay(n_ep - 1, False)

    @pl.loop(0, n_ep - 1)
    def _(c):
        scatter(c)

    finish(n_ep - 1)
    scatter(n_ep - 1)

    square = mixed[...] * mixed[...]
    lanes = square[:, :LANES]
    for k in range(1, width // LANES):
        lanes = lanes + square[:, k * LANES:(k + 1) * LANES]
    mine = jnp.sum(lanes.T, axis=0, keepdims=True)
    sums_out[...] = jnp.broadcast_to(mine, sums_out.shape)
    for step in range(1, n_tp):
        sum_copy(step).start()
    total = sums_out[...]
    for step in range(1, n_tp):
        source = (at + step) % n_tp
        remote(sums_out, sums_in.at[source], sum_send.at[step], sum_recv.at[source], me, source).wait_recv()
        total = total + sums_in[source]
    scale = lax.rsqrt(total / model_width + NORM_EPS)
    column = jnp.concatenate([scale] * (LANES // scale.shape[0]), axis=0).T
    for k in range(width // LANES):
        span = slice(k * LANES, (k + 1) * LANES)
        out_ref[:, span] = (mixed[:, span] * column * out_gain_ref[:, span]).astype(out_ref.dtype)

    for step in range(1, n_tp):
        sum_copy(step).wait_send()

    @pl.loop(0, n_ep)
    def _(c):
        @pl.when(c > 0)
        def _():
            pick_copy(c).wait_send()
            for h in range(pieces):
                back_copy(c, h).wait_send()

        @pl.loop(0, n_tp)
        def _(s):
            @pl.when(both(s <= at, at < last))
            def _():
                row_copy(c, s, 1).wait_send()

            @pl.when(both(s >= at, at > 0))
            def _():
                row_copy(c, s, 0).wait_send()

            for h in range(pieces):
                @pl.when(s > at)
                def _():
                    part_copy(c, s, h, 1).wait_send()

                @pl.when(s < at)
                def _():
                    part_copy(c, s, h, 0).wait_send()


def solution(mesh):
    n_ep, n_tp = mesh.shape["ep"], mesh.shape["tp"]

    def shards(tokens, pre_gain, out_gain, chosen, route_weight, expert_gate, expert_up, expert_down):
        tok_count, width = tokens.shape
        model_width = pre_gain.shape[0]
        slots, units = chosen.shape[2], expert_gate.shape[2]
        narrow = width // PIECES
        bf16, f32 = jnp.bfloat16, jnp.float32
        dma = pltpu.SemaphoreType.DMA
        vmem = pl.BlockSpec(memory_space=pltpu.VMEM)
        hbm = pl.BlockSpec(memory_space=pl.ANY)
        return pl.pallas_call(
            functools.partial(layer_kernel, n_ep, n_tp, model_width),
            out_shape=jax.ShapeDtypeStruct((tok_count, width), bf16),
            in_specs=[vmem] * 5 + [hbm] * 3,
            out_specs=vmem,
            scratch_shapes=[
                pltpu.VMEM((n_tp, width, units), bf16),
                pltpu.VMEM((n_tp, width, units), bf16),
                pltpu.VMEM((n_tp, PIECES, units, narrow), bf16),
                pltpu.VMEM((n_ep, n_tp, slots, width), bf16),
                pltpu.VMEM((n_ep, slots, width), bf16),
                pltpu.VMEM((n_ep, n_tp, PIECES, slots, narrow), f32),
                pltpu.VMEM((n_ep, n_tp, PIECES, slots, narrow), bf16),
                pltpu.VMEM((2, n_ep, n_tp, PIECES, slots, narrow), bf16),
                pltpu.VMEM((slots, units), f32),
                pltpu.VMEM((slots, units), f32),
                pltpu.VMEM((slots, 1), f32),
                pltpu.VMEM((slots, units), bf16),
                pltpu.VMEM((n_ep, PIECES, slots, narrow), bf16),
                pltpu.VMEM((n_ep, PIECES, slots, narrow), bf16),
                pltpu.VMEM((tok_count, width), f32),
                pltpu.VMEM((8, tok_count), f32),
                pltpu.VMEM((n_tp, 8, tok_count), f32),
                dma((n_tp,)), dma((n_tp,)), dma((n_tp, PIECES)),
                dma((n_ep,)), dma((n_ep,)),
                dma((2, n_ep, n_tp)), dma((n_ep, n_tp)),
                dma((n_ep, n_tp, PIECES)), dma((2, n_ep, n_tp, PIECES)),
                dma((n_ep, PIECES)), dma((n_ep, PIECES)),
                dma((n_tp,)), dma((n_tp,)),
            ],
            compiler_params=pltpu.CompilerParams(
                collective_id=0, has_side_effects=True, vmem_limit_bytes=67043328
            ),
        )(
            tokens, pre_gain.reshape(1, -1), out_gain.reshape(1, -1), chosen, route_weight,
            expert_gate, expert_up, expert_down,
        )

    return jax.shard_map(
        shards,
        mesh=mesh,
        in_specs=(
            P(("grp", "ep"), "tp"),
            P(),
            P("tp"),
            P(("grp", "ep"), None, None),
            P(("grp", "ep"), None, None),
            P("ep", None, "tp"),
            P("ep", None, "tp"),
            P("ep", "tp", None),
        ),
        out_specs=P(("grp", "ep"), "tp"),
        check_vma=False,
    )
```
